32 devices in a mesh: grp: 2 (over y), fs: 4 (over z), tp: 4 (over x, core).
Axes of the slice: x: 2, y: 2, z: 4, core: 2. Of those that a mesh axis runs over, the one named last changes fastest.
Arguments:
- tokens: bfloat16 [1024, 2048], P(('grp', 'fs')), parts along dimension 0, may hold values from -6 to 6
- pre_attention_gain: float32 [2048], replicated, may hold values from 0.1 to 1.9
- query_weight: bfloat16 [2048, 512], P('fs', 'tp'), may hold values from -0.125 to 0.125
- key_weight: bfloat16 [2048, 512], P('fs', 'tp'), may hold values from -0.125 to 0.125
- value_weight: bfloat16 [2048, 1024], P('fs', 'tp'), may hold values from -0.125 to 0.125
- output_gate_weight: bfloat16 [2048, 1024], P('fs', 'tp'), may hold values from -0.125 to 0.125
- decay_weight: bfloat16 [2048, 512], P('fs', 'tp'), may hold values from -0.25 to 0.25
- decay_logit_bias: float32 [512], P('tp'), may hold values from -1 to 4
- extra_log_decay: float32 [1024, 512], P(('grp', 'fs'), 'tp'), parts along dimension 0, may hold values from -0.7 to 0
- head_norm_gain: float32 [1024], P('tp'), may hold values from 0.1 to 1.9
- attention_out_weight: bfloat16 [1024, 2048], P('tp', 'fs'), may hold values from -0.1875 to 0.1875
- post_attention_gain: float32 [2048], replicated, may hold values from 0.1 to 1.9
- pre_feedforward_gain: float32 [2048], replicated, may hold values from 0.1 to 1.9
- post_feedforward_gain: float32 [2048], replicated, may hold values from 0.1 to 1.9
- up_weight: bfloat16 [2048, 8192], P('fs', 'tp'), may hold values from -0.125 to 0.125
- down_weight: bfloat16 [8192, 2048], P('tp', 'fs'), may hold values from -0.0625 to 0.0625
Outputs:
- layer_out: bfloat16 [1024, 2048], P(('grp', 'fs')), parts along dimension 0
The draws below stay inside these ranges and needn't reach their ends.
There are 2 independent parts, one for each index of `grp`. The reference program is written for one: setup_inputs(seed, part) draws one part's arguments, and reference() takes and returns one part's arrays. A program takes and returns all parts, laid end to end along the dimension named above; an argument that names none is the same for every part. Nothing has to cross between parts.
All inputs are finite; a program needn't handle non-finite values.
Results may differ from the reference program's by a relative error of at most 0.035.
Values may be sent and summed in bfloat16 or wider, within the bound.
A program may use at most 64 MiB of HBM per device.

```python
import jax
import jax.numpy as jnp
from jax import lax

D = 2048
HEADS = 8
DK = 64
DV = 128
BLOCK = 64
TOK_DEV = 128
QK = 512
V = 1024
FF = 8192
TOKENS = 512
N_TP = 4


def draw_extra_log_decay(key, part):
    first, second = jax.random.split(jax.random.fold_in(key, 11))
    chance = jax.random.uniform(first, (TOKENS, 1), jnp.float32)
    depth = jax.random.uniform(second, (TOKENS, QK), jnp.float32, minval=-0.7, maxval=-0.22)
    return jnp.where(chance < 3.0 / TOK_DEV, depth, 0.0).astype(jnp.float32)


def level_of(stream_key, extent, cuts, smallest, high):
    factor_of, own = 1.0, jax.random.fold_in(stream_key, 6)
    for axis_at, parts in cuts:
        heights = jnp.exp(jax.random.uniform(jax.random.fold_in(own, axis_at), (parts,), jnp.float32, smallest / len(cuts), high / len(cuts)))
        factor_of = factor_of * jnp.repeat(heights, extent[axis_at] // parts).reshape([-1 if axis == axis_at else 1 for axis in range(len(extent))])
    return factor_of


def scatter_about(own_key, shape, scale, limit, cuts=(), held_as=jnp.bfloat16):
    values = jax.random.normal(own_key, shape, jnp.float32) * scale
    if len(cuts) > 0:
        values = level_of(own_key, shape, cuts, -0.22, 0.18) * values
    return jnp.clip(values, min=-limit, max=limit).astype(held_as)


def setup_inputs(seed: int = 0, part: int = 0) -> dict:
    keys = jax.random.split(jax.random.key(seed), 17)
    own_keys = jax.random.split(jax.random.fold_in(keys[16], part), 17)
    return {
        "tokens": scatter_about(own_keys[0], (TOKENS, D), 1.0, 6.0, ((0, 4),)),
        "pre_attention_gain": jnp.clip(1.0 + 0.18 * jax.random.normal(keys[1], (D,), jnp.float32), 0.1, 1.9),
        "query_weight": scatter_about(keys[2], (D, QK), D ** -0.5, 0.125, ((0, 4), (1, 4))),
        "key_weight": scatter_about(keys[3], (D, QK), D ** -0.5, 0.125, ((0, 4), (1, 4))),
        "value_weight": scatter_about(keys[4], (D, V), D ** -0.5, 0.125, ((0, 4), (1, 4))),
        "output_gate_weight": scatter_about(keys[5], (D, V), D ** -0.5, 0.125, ((0, 4), (1, 4))),
        "decay_weight": scatter_about(keys[6], (D, QK), (D // 4) ** -0.5, 0.25, ((0, 4), (1, 4))),
        "decay_logit_bias": jnp.clip(-1.0 + 5.0 * jax.random.uniform(keys[7], (QK,), jnp.float32) ** level_of(keys[7], (QK,), ((0, 4),), -0.2, 0.2), -1.0, 4.0),
        "extra_log_decay": draw_extra_log_decay(jax.random.fold_in(jax.random.fold_in(keys[16], part), 71), part),
        "head_norm_gain": jnp.clip(1.0 + 0.18 * jax.random.normal(keys[9], (V,), jnp.float32), 0.1, 1.9),
        "attention_out_weight": scatter_about(keys[10], (V, D), V ** -0.5, 0.1875, ((0, 4), (1, 4))),
        "post_attention_gain": jnp.clip(1.0 + 0.18 * jax.random.normal(keys[11], (D,), jnp.float32), 0.1, 1.9),
        "pre_feedforward_gain": jnp.clip(1.0 + 0.18 * jax.random.normal(keys[12], (D,), jnp.float32), 0.1, 1.9),
        "post_feedforward_gain": jnp.clip(1.0 + 0.18 * jax.random.normal(keys[13], (D,), jnp.float32), 0.1, 1.9),
        "up_weight": scatter_about(keys[14], (D, FF), D ** -0.5, 0.125, ((0, 4), (1, 4))),
        "down_weight": scatter_about(keys[15], (FF, D), FF ** -0.5, 0.0625, ((0, 4), (1, 4))),
    }


EPS = 1e-06
GATE_NORM_SCALE = 16.0
HIGH = lax.Precision.HIGHEST

def root_norm(rows, gain):
    values = rows.astype(jnp.float32)
    return values * lax.rsqrt(lax.optimization_barrier(jnp.mean(values * values, axis=-1, keepdims=True)) + EPS) * gain

def decayed_attention(queries, keys_in, values_in, decay_log_rate):
    length, heads, key_dim = queries.shape
    value_dim = values_in.shape[-1]
    blocks = length // BLOCK

    def to_blocks(array):
        return array.reshape(blocks, BLOCK, heads, array.shape[-1]).transpose(0, 2, 1, 3)
    query_blocks = to_blocks(queries)
    key_blocks = to_blocks(keys_in)
    value_blocks = to_blocks(values_in)
    cumulative = jnp.cumsum(to_blocks(decay_log_rate), axis=2)
    causal = jnp.tril(jnp.ones((BLOCK, BLOCK), dtype=bool))[:, :, None]

    def advance(state, inputs):
        query_blk, key_blk, value_blk, cum_blk = inputs
        relative = cum_blk[:, :, None, :] - cum_blk[:, None, :, :]
        weights = jnp.exp(jnp.where(causal, relative, -jnp.inf))
        scores = jnp.einsum('hid,hjd,hijd->hij', query_blk, key_blk, weights, precision=HIGH)
        inner = jnp.einsum('hij,hjv->hiv', scores, value_blk, precision=HIGH)
        inner = inner + jnp.einsum('hid,hdv->hiv', query_blk * jnp.exp(cum_blk), state, precision=HIGH)
        last = cum_blk[:, -1:, :]
        state = state * jnp.exp(last)[:, 0, :, None] + jnp.einsum('hjd,hjv->hdv', key_blk * jnp.exp(last - cum_blk), value_blk, precision=HIGH)
        return (state, inner)
    initial = jnp.zeros((heads, key_dim, value_dim), jnp.float32)
    _, result = lax.scan(advance, initial, (query_blocks, key_blocks, value_blocks, cumulative))
    return result.transpose(0, 2, 1, 3).reshape(length, heads, value_dim)

def grouped_sum(left, right, groups):
    width = left.shape[1] // groups

    def add_group(index, total):
        start = (index * width).astype(jnp.int32)
        cols = lax.dynamic_slice_in_dim(left, start, width, 1)
        rows = lax.dynamic_slice_in_dim(right, start, width, 0)
        part = jnp.dot(cols, rows, preferred_element_type=jnp.float32)
        rounded = lax.optimization_barrier(part.astype(jnp.bfloat16))
        return total + rounded.astype(jnp.float32)
    empty = jnp.zeros((left.shape[0], right.shape[1]), jnp.float32)
    return lax.fori_loop(jnp.int32(0), jnp.int32(groups), add_group, empty)

def reference(tokens, pre_attention_gain, query_weight, key_weight, value_weight, output_gate_weight, decay_weight, decay_logit_bias, extra_log_decay, head_norm_gain, attention_out_weight, post_attention_gain, pre_feedforward_gain, post_feedforward_gain, up_weight, down_weight):
    stream_in = tokens.astype(jnp.float32)
    normed = root_norm(stream_in, pre_attention_gain).astype(jnp.bfloat16)
    query_rows = jnp.dot(normed, query_weight, preferred_element_type=jnp.float32).astype(jnp.bfloat16)
    key_rows = jnp.dot(normed, key_weight, preferred_element_type=jnp.float32).astype(jnp.bfloat16)
    value_rows = jnp.dot(normed, value_weight, preferred_element_type=jnp.float32).astype(jnp.bfloat16)
    gate_rows = jnp.dot(normed, output_gate_weight, preferred_element_type=jnp.float32).astype(jnp.bfloat16)
    decay_logits = jnp.dot(normed, decay_weight, preferred_element_type=jnp.float32)
    decay_log_rate = jax.nn.log_sigmoid(decay_logits + decay_logit_bias) / GATE_NORM_SCALE + extra_log_decay
    seqs = TOKENS // TOK_DEV
    queries = (query_rows.astype(jnp.float32) * DK ** (-0.5)).reshape(seqs, TOK_DEV, HEADS, DK)
    keys_in = key_rows.astype(jnp.float32).reshape(seqs, TOK_DEV, HEADS, DK)
    values_in = value_rows.astype(jnp.float32).reshape(seqs, TOK_DEV, HEADS, DV)
    decays = decay_log_rate.reshape(seqs, TOK_DEV, HEADS, DK)
    attended = lax.map(lambda item: decayed_attention(*item), (queries, keys_in, values_in, decays))
    attended = attended.reshape(TOKENS, HEADS, DV)
    scaled = attended * lax.rsqrt(lax.optimization_barrier(jnp.mean(attended * attended, axis=-1, keepdims=True)) + EPS)
    scaled = scaled.reshape(TOKENS, V) * head_norm_gain
    headout = (scaled * jax.nn.silu(gate_rows.astype(jnp.float32))).astype(jnp.bfloat16)
    mixed = grouped_sum(headout, attention_out_weight, N_TP)
    stream = stream_in + root_norm(mixed, post_attention_gain)
    normed_mid = root_norm(stream, pre_feedforward_gain).astype(jnp.bfloat16)
    hidden = jnp.square(jax.nn.relu(jnp.dot(normed_mid, up_weight, preferred_element_type=jnp.float32))).astype(jnp.bfloat16)
    feedfwd = grouped_sum(hidden, down_weight, N_TP)
    return (stream + root_norm(feedfwd, post_feedforward_gain)).astype(jnp.bfloat16)
```

```python
import math

import jax
import jax.numpy as jnp
from jax import lax
from jax.experimental import pallas as pl
from jax.experimental.pallas import tpu as pltpu
from jax.sharding import PartitionSpec as P

DK = 64
DV = 128
EPS = 1e-06
GATE_NORM_SCALE = 16.0


def root_norm(rows, gain):
    return rows * lax.rsqrt(jnp.mean(rows * rows, axis=-1, keepdims=True) + EPS) * gain


def split2(x):
    hi = x.astype(jnp.bfloat16)
    lo = (x - hi.astype(jnp.float32)).astype(jnp.bfloat16)
    return hi, lo


def dot_t(a, b):
    return lax.dot_general(a, b, (((1,), (1,)), ((), ())), preferred_element_type=jnp.float32)


def split3(x):
    hi = x.astype(jnp.bfloat16)
    rest = x - hi.astype(jnp.float32)
    mid = rest.astype(jnp.bfloat16)
    return hi, mid, (rest - mid.astype(jnp.float32)).astype(jnp.bfloat16)


def pick(mask, parts):
    chosen = mask.astype(jnp.float32).astype(jnp.bfloat16)
    total = 0.0
    for part in parts:
        total = total + jnp.dot(chosen, part, preferred_element_type=jnp.float32)
    return total


def attend(q, k, v, log_decay):
    n, width = q.shape
    heads = width // DK
    row = lax.broadcasted_iota(jnp.int32, (n, n), 0)
    col = lax.broadcasted_iota(jnp.int32, (n, n), 1)
    lane = lax.broadcasted_iota(jnp.int32, (n, width), 1)
    cum = pick(row >= col, split3(log_decay))
    cum_parts = split3(cum)

    def per_head(x):
        return jnp.concatenate(
            [jnp.where((lane >= h * DK) & (lane < (h + 1) * DK), x, 0.0) for h in range(heads)], 0
        )

    def scores_of(left, right):
        lh, ll = split2(per_head(left))
        rh, rl = split2(right)
        return dot_t(lh, rh) + dot_t(lh, rl) + dot_t(ll, rh)

    tiled_row = jnp.concatenate([row] * heads, 0)
    tiled_col = jnp.concatenate([col] * heads, 0)
    scores = jnp.where(
        tiled_row == tiled_col,
        dot_t(per_head(q).astype(jnp.bfloat16), k.astype(jnp.bfloat16)),
        0.0,
    )
    half = n // 2
    while half >= 1:
        bound = pick(col == (row & ~(2 * half - 1)) + (half - 1), cum_parts)
        fade = jnp.exp(-jnp.abs(cum - bound))
        part = scores_of(q * fade, k * fade)
        apart = tiled_row ^ tiled_col
        keep = (apart >= half) & (apart < 2 * half) & (tiled_row > tiled_col)
        scores = jnp.where(keep, part, scores)
        half //= 2
    outs = []
    for h in range(heads):
        sh, sl = split2(scores[h * n : (h + 1) * n])
        vh = v[:, h * DV : (h + 1) * DV]
        outs.append(
            jnp.dot(sh, vh, preferred_element_type=jnp.float32)
            + jnp.dot(sl, vh, preferred_element_type=jnp.float32)
        )
    return outs


def head_block(acc, bias, extra, gain, qk, v):
    bf = jnp.bfloat16
    q = acc[:, :qk].astype(bf).astype(jnp.float32) * DK ** (-0.5)
    k = acc[:, qk : 2 * qk].astype(bf).astype(jnp.float32)
    x = acc[:, 2 * qk : 3 * qk] + bias
    log_sig = jnp.minimum(x, 0.0) - jnp.log1p(jnp.exp(-jnp.abs(x)))
    rate = log_sig / GATE_NORM_SCALE + extra
    vals = acc[:, 3 * qk : 3 * qk + v].astype(bf)
    gate = acc[:, 3 * qk + v :].astype(bf).astype(jnp.float32)
    outs = attend(q, k, vals, rate)
    scaled = jnp.concatenate(
        [o * lax.rsqrt(jnp.mean(o * o, axis=-1, keepdims=True) + EPS) for o in outs], 1
    )
    return (scaled * gain * (gate / (1.0 + jnp.exp(-gate)))).astype(bf)


def local_plain(
    tokens, pre_attention_gain, query_weight, key_weight, value_weight, output_gate_weight,
    decay_weight, decay_logit_bias, extra_log_decay, head_norm_gain, attention_out_weight,
    post_attention_gain, pre_feedforward_gain, post_feedforward_gain, up_weight, down_weight,
):
    bf = jnp.bfloat16
    n_fs = lax.axis_size("fs")
    n_tp = lax.axis_size("tp")
    length, width = tokens.shape
    share = length // n_tp
    cols = width // n_fs
    qk, v = query_weight.shape[1], value_weight.shape[1]
    stream_in = tokens.astype(jnp.float32)
    normed = root_norm(stream_in, pre_attention_gain).astype(bf)
    joined = jnp.concatenate(
        [query_weight, key_weight, decay_weight, value_weight, output_gate_weight], 1
    )
    whole = lax.all_gather(joined, "fs", axis=0, tiled=True)
    acc = jnp.dot(normed, whole, preferred_element_type=jnp.float32)
    headout = head_block(acc, decay_logit_bias, extra_log_decay, head_norm_gain, qk, v)
    whole_out = lax.all_gather(attention_out_weight, "fs", axis=1, tiled=True)
    mix_part = jnp.dot(headout, whole_out, preferred_element_type=jnp.float32).astype(bf)
    mix = lax.all_to_all(
        mix_part.reshape(n_tp, share, width), "tp", split_axis=0, concat_axis=0, tiled=True
    )
    mixed = jnp.sum(mix.astype(jnp.float32), 0)
    mine = lax.dynamic_slice_in_dim(stream_in, lax.axis_index("tp") * share, share, 0)
    stream = mine + root_norm(mixed, post_attention_gain)
    normed_mid = root_norm(stream, pre_feedforward_gain).astype(bf)
    blocks = normed_mid.reshape(share, n_fs, cols).transpose(1, 0, 2)
    blocks = lax.all_to_all(blocks, "fs", split_axis=0, concat_axis=0, tiled=True)
    rows = lax.all_gather(blocks, "tp", axis=1, tiled=True)
    up = jnp.dot(rows.reshape(n_fs * length, cols), up_weight, preferred_element_type=jnp.float32)
    up = up.astype(bf).reshape(n_fs, length, -1)
    up = lax.all_to_all(up, "fs", split_axis=0, concat_axis=0, tiled=True)
    hidden = jnp.square(jax.nn.relu(jnp.sum(up.astype(jnp.float32), 0))).astype(bf)
    hidden = lax.all_gather(hidden, "fs", axis=0, tiled=True)
    down = jnp.dot(hidden, down_weight, preferred_element_type=jnp.float32).astype(bf)
    down = down.reshape(n_fs, n_tp, share, cols).transpose(1, 0, 2, 3)
    down = lax.all_to_all(down, "tp", split_axis=0, concat_axis=0, tiled=True)
    feed = jnp.sum(down.astype(jnp.float32), 0).astype(bf)
    feed = lax.all_to_all(feed, "fs", split_axis=0, concat_axis=0, tiled=True)
    feed = feed.transpose(1, 0, 2).reshape(share, width).astype(jnp.float32)
    out = (stream + root_norm(feed, post_feedforward_gain)).astype(bf)
    return lax.all_gather(out, "tp", axis=0, tiled=True)


def exchange_kernel(
    x_ref, q_ref, k_ref, d_ref, v_ref, g_ref, bias_ref, extra_ref, head_gain_ref, wo_ref,
    gain_a_ref, gain_b_ref, gain_c_ref, gain_d_ref, up_ref, down_ref, out_ref,
    nm, no, qp, kp, dp, vp, gp, p1s, p2s, p1r, p2r, wop, mixs, mixr, st, am, upf, dnf, hid,
    part, from_sib, to_x, from_x, to_pair, from_pair, to_far, from_far, to_late, from_late, ff,
    here, send, recv,
    *, n_fs, n_tp, qk, v,
):
    bf, f32 = jnp.bfloat16, jnp.float32
    g, f, t = lax.axis_index("grp"), lax.axis_index("fs"), lax.axis_index("tp")
    pair, far, b, half = f ^ 1, f ^ 2, f & 1, f >> 1
    share = out_ref.shape[1]
    cols = st.shape[2]
    length = n_tp * share
    count = [0]
    groups = {}

    def slots(n):
        first = count[0]
        count[0] += n
        return first

    def put(src, dst, at, group, **where):
        sem, sizes = groups.setdefault(group, (len(groups), []))
        sizes.append(math.prod(src.shape))
        pltpu.make_async_remote_copy(
            src_ref=src, dst_ref=dst, send_sem=send.at[sem], recv_sem=recv.at[at],
            device_id=where, device_id_type=pl.DeviceIdType.MESH,
        ).start()

    def copy_like(ref, sem, at):
        return pltpu.make_async_remote_copy(
            src_ref=ref, dst_ref=ref, send_sem=send.at[sem], recv_sem=recv.at[at],
            device_id={"fs": far}, device_id_type=pl.DeviceIdType.MESH,
        )

    def take(dst, at):
        copy_like(dst, 0, at).wait_recv()

    def sent(group, like):
        sem, sizes = groups.pop(group)
        groups[(group, "sent")] = (sem, None)
        assert sum(sizes) == math.prod(like.shape), (group, sum(sizes))
        copy_like(like, sem, 0).wait_send()

    def dot(l, r):
        return jnp.dot(l, r, preferred_element_type=f32)

    def squares(blocks):
        total = 0.0
        for block in blocks:
            total = total + jnp.sum(block * block, axis=-1, keepdims=True)
        return lax.rsqrt(total / (n_fs * cols) + EPS)

    def rows_of(ref, at):
        return ref[:, at].reshape(length, cols)

    hid_cols = upf.shape[2]
    own_up = pltpu.make_async_copy(
        up_ref.at[:, pl.ds(pl.multiple_of(f * hid_cols, hid_cols), hid_cols)], upf.at[f], here.at[0]
    )
    own_down = pltpu.make_async_copy(
        down_ref.at[pl.ds(pl.multiple_of(f * hid_cols, hid_cols), hid_cols)], dnf.at[f], here.at[1]
    )
    own_up.start()
    own_down.start()

    barrier = pltpu.get_barrier_semaphore()
    peers = [{"grp": 1 - g}]
    peers += [{"fs": f ^ s} for s in range(1, n_fs)]
    peers += [{"tp": t ^ k} for k in range(1, n_tp)]
    for peer in peers:
        pl.semaphore_signal(barrier, inc=1, device_id=peer, device_id_type=pl.DeviceIdType.MESH)
    pl.semaphore_wait(barrier, len(peers))

    class Fetch:
        def __init__(self, ref, into, pieces, group):
            self.ref, self.into, self.pieces, self.group = ref, into, pieces, group
            self.at = slots(pieces + 1)
            self.size = ref.shape[0] // (2 * pieces)

        def piece(self, ref, side, i):
            at = pl.multiple_of(side * (self.pieces * self.size) + i * self.size, self.size)
            return ref.at[pl.ds(at, self.size)]

        def start(self):
            for i in range(self.pieces):
                put(
                    self.piece(self.ref, g, i), self.piece(self.into, g, i), self.at + 1 + i,
                    self.group, fs=pair,
                )

        def pass_on(self):
            for i in range(self.pieces):
                mine = self.piece(self.into, g, i)
                take(mine, self.at + 1 + i)
                put(mine, mine, self.at, self.group, grp=1 - g)

        def settle(self):
            rows = self.pieces * self.size
            take(self.into.at[pl.ds(pl.multiple_of((1 - g) * rows, rows), rows)], self.at)

    class Spread:
        def __init__(self, source, spot, group):
            self.source, self.spot, self.group = source, spot, group
            self.pieces = 2
            self.at = slots(n_fs * (self.pieces + 1))
            self.size = hid_cols // (2 * self.pieces)

        def sem(self, s, i):
            return self.at + s * (self.pieces + 1) + i

        def chunk(self, side, i):
            return pl.ds(pl.multiple_of((side * self.pieces + i) * self.size, self.size), self.size)

        def start(self, s, i):
            at = self.chunk(g, i)
            put(self.source(f ^ s, at), self.spot(f, at), self.sem(s, i), self.group, fs=f ^ s)

        def pass_on(self, s, i):
            mine = self.spot(f ^ s, self.chunk(g, i))
            take(mine, self.sem(s, i))
            put(mine, mine, self.sem(s, self.pieces), self.group, grp=1 - g)

        def settle(self, s):
            wide = self.pieces * self.size
            at = pl.ds(pl.multiple_of((1 - g) * wide, wide), wide)
            take(self.spot(f ^ s, at), self.sem(s, self.pieces))

    def units_of(to):
        return pl.ds(pl.multiple_of(to * hid_cols, hid_cols), hid_cols)

    up = Spread(lambda to, at: up_ref.at[at, units_of(to)], lambda c, at: upf.at[c, at], "up")
    down = Spread(lambda to, at: down_ref.at[units_of(to), at], lambda c, at: dnf.at[c, :, at], "down")
    weights = [q_ref, k_ref, d_ref, v_ref, g_ref]
    fetches = [
        Fetch(r, p, n, group)
        for r, p, n, group in zip(
            weights, (qp, kp, dp, vp, gp), (1, 1, 1, 2, 2), ("qk", "qk", "qk", "v", "v")
        )
    ]

    def normalize(rows, into, at):
        blocks = [rows[:, c * cols : (c + 1) * cols].astype(f32) for c in range(n_fs)]
        scale = squares(blocks)
        for c in range(n_fs):
            into[at, c] = (blocks[c] * scale * gain_a_ref[c]).astype(bf)

    wo_at = slots(n_fs)
    rows_wo = wo_ref.shape[0] // 2

    def wo_part(ref, side):
        return ref.at[pl.ds(pl.multiple_of(side * rows_wo, rows_wo), rows_wo)]

    def wo_start(s):
        put(wo_part(wo_ref, g), wo_part(wop.at[f], g), wo_at + s, "wo", fs=f ^ s)

    def wo_pass(s):
        mine = wo_part(wop.at[f ^ s], g)
        take(mine, wo_at + s)
        if s == 2:
            put(mine, mine, wo_at + 3, "wo", fs=pair)
        put(mine, mine, wo_at, "wo", grp=1 - g)

    normalize(x_ref[t], nm, t)
    no_at = slots(2)
    put(nm.at[t, pl.ds(2 * (1 - half), 2)], no.at[t], no_at, "no", fs=far)
    for fetch in fetches:
        fetch.start()
    wo_start(2)
    wo_start(1)
    for k in range(1, n_tp):
        normalize(x_ref[t ^ k], nm, t ^ k)

    fetches[0].pass_on()
    take(no.at[t], no_at)
    for k in (2, 3, 1):
        put(no.at[t], no.at[t], no_at + 1, "no", tp=t ^ k)
    fetches[1].pass_on()
    fetches[2].pass_on()
    take(no.at[pl.ds(0, n_tp - 1)], no_at + 1)
    no_own, no_pair = rows_of(no, b), rows_of(no, 1 - b)
    outgoing = [p1s.at[0], p1s.at[1], p1s.at[2], p2s.at[0], p2s.at[1]]
    incoming = [p1r.at[0], p1r.at[1], p1r.at[2], p2r.at[0], p2r.at[1]]
    part_at = slots(2)

    def far_part(i):
        fetches[i].settle()
        outgoing[i][...] = (
            dot(no_own, weights[i][...]) + dot(no_pair, fetches[i].into[...])
        ).astype(bf)
        late = i // 3
        put(outgoing[i], incoming[i], part_at + late, ("p1", "p2")[late], fs=far)

    far_part(0)
    far_part(1)
    fetches[3].pass_on()
    far_part(2)
    fetches[4].pass_on()
    nm_own, nm_pair = rows_of(nm, f), rows_of(nm, pair)

    def own_part(i):
        return dot(nm_own, weights[i][...]) + dot(nm_pair, fetches[i].into[...])

    acc = [own_part(0), own_part(1), own_part(2)]
    far_part(3)
    wo_pass(2)
    far_part(4)
    wo_pass(1)
    for s, i in ((1, 0), (1, 1), (2, 0), (3, 0), (2, 1)):
        up.start(s, i)
    acc += [own_part(3), own_part(4)]
    take(p1r, part_at)
    wo_pass(3)
    take(p2r, part_at + 1)
    acc = [mine + other[...].astype(f32) for mine, other in zip(acc, incoming)]
    headout = head_block(
        jnp.concatenate(acc, 1), bias_ref[...], extra_ref[...], head_gain_ref[...], qk, v
    )

    def mix_block(s):
        weight = wo_ref[...] if s == 0 else wop[f ^ s]
        block = dot(headout, weight).astype(bf)
        for k in range(n_tp):
            mixs[k ^ t, f ^ s] = block[k * share : (k + 1) * share]

    up.pass_on(1, 0)
    mix_block(0)
    take(wop.at[pl.ds(0, n_fs - 1), pl.ds(0, rows_wo)], wo_at)
    for s in (1, 2, 3):
        mix_block(s)
    mix_at = slots(n_tp)
    put(mixs.at[3], mixr.at[3], mix_at + 3, "mix", tp=t ^ 1)
    put(mixs.at[1], mixr.at[1], mix_at + 1, "mix", tp=t ^ 1)
    take(mixr.at[3], mix_at + 3)
    mixr[0] = (mixs[2].astype(f32) + mixr[3].astype(f32)).astype(bf)
    put(mixr.at[0], mixr.at[2], mix_at + 2, "mix", tp=t ^ 2)
    mine = [x_ref[t, :, c * cols : (c + 1) * cols].astype(f32) for c in range(n_fs)]
    up.pass_on(1, 1)
    take(mixr.at[1], mix_at + 1)
    take(mixr.at[2], mix_at + 2)
    mix = mixs[0].astype(f32) + mixr[1].astype(f32) + mixr[2].astype(f32)
    mix = [mix[c] for c in range(n_fs)]
    scale = squares(mix)
    stream = [mine[c] + mix[c] * scale * gain_b_ref[c] for c in range(n_fs)]
    scale = squares(stream)
    for c in range(n_fs):
        st[c] = stream[c]
        am[0, 0, c] = (stream[c] * scale * gain_c_ref[c]).astype(bf)

    mid_z, mid_x, mid_sib = slots(n_fs), slots(n_fs), slots(n_fs)

    def mid_over(k):
        put(am.at[k, 0], am.at[k, 2], mid_x + k, "mid", tp=t ^ 2)
        put(am.at[k, 0], am.at[k, 1], mid_sib + k, "mid", tp=t ^ 1)

    def mid_across(k):
        take(am.at[k, 2], mid_x + k)
        put(am.at[k, 2], am.at[k, 3], mid_sib + k, "mid", tp=t ^ 1)

    put(am.at[0, 0], am.at[2, 0], mid_z + 2, "mid_z", fs=far)
    put(am.at[0, 0], am.at[1, 0], mid_z + 1, "mid_z", fs=pair)
    mid_over(0)
    up.start(3, 1)
    up.pass_on(2, 0)
    up.pass_on(3, 0)
    up.pass_on(2, 1)
    take(am.at[2, 0], mid_z + 2)
    put(am.at[2, 0], am.at[3, 0], mid_z + 3, "mid_z", fs=pair)
    for s, i in ((1, 0), (1, 1), (2, 0), (2, 1), (3, 0), (3, 1)):
        down.start(s, i)
    mid_over(2)
    take(am.at[1, 0], mid_z + 1)
    mid_over(1)
    mid_across(0)
    sent("qk", am.at[0, pl.ds(0, 3)])
    sent("v", am.at[0])
    sent("no", am.at[0, pl.ds(0, 2)])
    sent("wo", wop.at[pl.ds(0, 3)])
    sent("p1", p1s)
    sent("p2", p2s)
    sent("mix", mixs.at[pl.ds(0, 3)])
    up.pass_on(3, 1)
    take(am.at[3, 0], mid_z + 3)
    mid_over(3)
    mid_across(2)
    mid_across(1)
    for s in (1, 2, 3):
        up.settle(s)
    own_up.wait()

    def raise_rows(k):
        take(am.at[k, pl.ds(0, 2)], mid_sib + k)
        total = 0.0
        for c in range(n_fs):
            total = total + dot(am[k, :, c].reshape(length, cols), upf[c])
        total = jnp.maximum(total, 0.0)
        hid[k] = (total * total).astype(bf)

    raise_rows(0)
    raise_rows(2)
    down.pass_on(1, 0)
    raise_rows(1)
    mid_across(3)
    down.pass_on(1, 1)
    raise_rows(3)
    own_down.wait()

    sib_at, x3_at, x_at = slots(2 * n_fs), slots(2 * n_fs), slots(2 * n_fs)
    pair_at, far_at, late_at = slots(2), slots(2) - 2, slots(4)
    hidden = hid[...].reshape(n_fs * length, hid_cols)
    wide = cols // 2

    def columns(side):
        at = g if side == 0 else 1 - g
        return pl.ds(pl.multiple_of(at * wide, wide), wide)

    def project(j, side):
        both = (0, 1) if side is None else (side,)
        for one in both:
            block = dot(hidden, dnf[f ^ j, :, columns(one)]).astype(bf)
            block = block.reshape(n_fs, n_tp, share, wide)
            for m in range(n_tp):
                part[j, m, one] = block[:, m]
        at = pl.ds(0, 2) if side is None else pl.ds(side, 1)
        sem = 2 * j + (side or 0)
        put(part.at[j, 3, at], from_sib.at[j, 1, at], x3_at + sem, "sib", tp=t ^ 1)
        put(part.at[j, 1, at], from_sib.at[j, 0, at], sib_at + sem, "sib", tp=t ^ 1)

    def over_x(j, side):
        at = pl.ds(0, 2) if side is None else pl.ds(side, 1)
        sem = 2 * j + (side or 0)
        take(from_sib.at[j, 1, at], x3_at + sem)
        to_x[j, at] = (part[j, 2, at].astype(f32) + from_sib[j, 1, at].astype(f32)).astype(bf)
        put(to_x.at[j, at], from_x.at[j, at], x_at + sem, "x", tp=t ^ 2)

    def summed(j, side, k):
        total = part[j, 0, side, k].astype(f32) + from_sib[j, 0, side, k].astype(f32)
        return total + from_x[j, side, k].astype(f32)

    def over_pair(j):
        take(from_sib.at[j, 0], sib_at + 2 * j)
        take(from_x.at[j], x_at + 2 * j)
        for k in (1, 3):
            for side in range(2):
                to_pair[j, k >> 1, side] = summed(j, side, k).astype(bf)
        put(to_pair.at[j], from_pair.at[j ^ 1], pair_at + (j ^ 1), "pair", fs=pair)
        for k in (0, 2):
            for side in range(2):
                ff[j, k >> 1, side] = summed(j, side, k)

    def over_far(j):
        take(from_pair.at[j], pair_at + j)
        to_far[j] = (ff[j, 1] + from_pair[j, 1].astype(f32)).astype(bf)
        put(to_far.at[j], from_far.at[j ^ 2], far_at + (j ^ 2), "far", fs=far)

    def direct(j, side):
        at = pl.ds(side, 1)
        take(from_sib.at[j, 0, at], sib_at + 2 * j + side)
        take(from_x.at[j, at], x_at + 2 * j + side)
        for k in (3, 2, 1):
            to_late[j - 2, side, k] = summed(j, side, k).astype(bf)
            put(
                to_late.at[j - 2, side, k], from_late.at[j - 2, side, k],
                late_at + 2 * (j - 2) + side, "late", fs=f ^ k,
            )
        ff[j, 0, side] = summed(j, side, 0)

    project(0, None)
    down.pass_on(2, 0)
    over_x(0, None)
    down.settle(1)
    project(1, None)
    down.pass_on(2, 1)
    over_x(1, None)
    project(2, 0)
    over_pair(0)
    over_x(2, 0)
    down.pass_on(3, 0)
    over_pair(1)
    down.settle(2)
    project(2, 1)
    over_far(0)
    over_x(2, 1)
    sent("up", upf.at[pl.ds(0, 3)])
    sent("mid", am.at[pl.ds(0, 3)])
    sent("mid_z", am.at[0, pl.ds(0, 3)])
    down.pass_on(3, 1)
    project(3, 0)
    direct(2, 0)
    over_x(3, 0)
    over_far(1)
    direct(2, 1)
    direct(3, 0)
    down.settle(3)
    project(3, 1)
    over_x(3, 1)
    sent("pair", to_pair.at[pl.ds(0, 2)])
    feed = [[ff[j, 0, side] for side in range(2)] for j in range(n_fs - 1)]
    feed.append([ff[3, 0, 0], None])
    for j in (0, 1):
        for side in range(2):
            feed[j][side] = feed[j][side] + from_pair[j, 0, side].astype(f32)
    for j in (2, 3):
        take(from_far.at[j], far_at + j)

    def add_late(j, side):
        take(from_late.at[j - 2, side, pl.ds(0, 3)], late_at + 2 * (j - 2) + side)
        for k in (1, 2, 3):
            feed[j ^ k][side] = feed[j ^ k][side] + from_late[j - 2, side, k].astype(f32)

    sent("down", dnf.at[pl.ds(0, 3)])
    sent("far", to_far.at[pl.ds(0, 2)])
    direct(3, 1)
    feed[3][1] = ff[3, 0, 1]
    for j in (2, 3):
        for side in range(2):
            feed[j][side] = feed[j][side] + from_far[j, side].astype(f32)
    for j, side in ((2, 0), (2, 1), (3, 0)):
        add_late(j, side)
    sent("sib", part.at[pl.ds(0, 2)])
    sent("x", to_x)
    add_late(3, 1)
    scale = squares([block for blocks in feed for block in blocks])
    for j in range(n_fs):
        for side in range(2):
            at = pl.ds(pl.multiple_of((f ^ j) * cols + (g ^ side) * wide, wide), wide)
            gained = feed[j][side] * scale * gain_d_ref[f ^ j, :, columns(side)]
            out_ref[t, :, at] = (st[f ^ j, :, columns(side)] + gained).astype(bf)
    out_at = slots(2)
    put(out_ref.at[t], out_ref.at[t], out_at, "out", tp=t ^ 2)
    put(out_ref.at[t], out_ref.at[t], out_at + 1, "out", tp=t ^ 1)
    sent("late", no.at[pl.ds(0, 3)])
    take(out_ref.at[t ^ 2], out_at)
    put(out_ref.at[t ^ 2], out_ref.at[t ^ 2], out_at + 1, "out", tp=t ^ 1)
    take(out_ref.at[pl.ds(0, 2)], out_at + 1)
    sent("out", mixs.at[pl.ds(0, 3)])
    assert count[0] <= recv.shape[0] and len(groups) <= send.shape[0], (count, len(groups))


def local_fused(
    tokens, pre_attention_gain, query_weight, key_weight, value_weight, output_gate_weight,
    decay_weight, decay_logit_bias, extra_log_decay, head_norm_gain, attention_out_weight,
    post_attention_gain, pre_feedforward_gain, post_feedforward_gain, up_weight, down_weight,
):
    bf, f32 = jnp.bfloat16, jnp.float32
    n_fs, n_tp = lax.axis_size("fs"), lax.axis_size("tp")
    length, width = tokens.shape
    share, cols = length // n_tp, width // n_fs
    qk, v = query_weight.shape[1], value_weight.shape[1]
    mine = up_weight.shape[1] // n_fs
    vm = pltpu.VMEM
    block = (n_fs, share, cols)
    sides, rows = (2,), (n_fs, share, cols // 2)
    scratch = [
        vm((n_tp,) + block, bf), vm((n_tp, 2, share, cols), bf),
        vm(query_weight.shape, bf), vm(key_weight.shape, bf), vm(decay_weight.shape, bf),
        vm(value_weight.shape, bf), vm(output_gate_weight.shape, bf),
        vm((3, length, qk), bf), vm((2, length, v), bf),
        vm((3, length, qk), bf), vm((2, length, v), bf),
        vm((n_fs,) + attention_out_weight.shape, bf),
        vm((n_tp,) + block, bf), vm((n_tp,) + block, bf), vm(block, f32),
        vm((n_fs, n_tp) + block, bf),
        vm((n_fs, cols, mine), bf), vm((n_fs, mine, cols), bf),
        vm((n_fs, length, mine), bf),
        vm((n_fs, n_tp) + sides + rows, bf), vm((n_fs, 2) + sides + rows, bf),
        vm((n_fs,) + sides + rows, bf), vm((n_fs,) + sides + rows, bf),
        vm((n_fs, 2, 2) + rows[1:], bf), vm((n_fs, 2, 2) + rows[1:], bf),
        vm((n_fs, 2) + rows[1:], bf), vm((n_fs, 2) + rows[1:], bf),
        vm((2,) + sides + rows, bf), vm((2,) + sides + rows, bf),
        vm((n_fs, 2, 2) + rows[1:], f32),
        pltpu.SemaphoreType.DMA((2,)),
        pltpu.SemaphoreType.DMA((20,)), pltpu.SemaphoreType.DMA((100,)),
    ]

    def kernel(*refs):
        exchange_kernel(*refs, n_fs=n_fs, n_tp=n_tp, qk=qk, v=v)

    def gain_blocks(gain):
        return gain.reshape(n_fs, 1, cols)

    vmem, anywhere = pl.BlockSpec(memory_space=pltpu.VMEM), pl.BlockSpec(memory_space=pl.ANY)
    out = pl.pallas_call(
        kernel,
        out_shape=jax.ShapeDtypeStruct((n_tp, share, width), bf),
        in_specs=[vmem] * 14 + [anywhere] * 2,
        out_specs=vmem,
        scratch_shapes=scratch,
        compiler_params=pltpu.CompilerParams(
            collective_id=0, has_side_effects=True, vmem_limit_bytes=60 * 2**20
        ),
    )(
        tokens.reshape(n_tp, share, width), query_weight, key_weight, decay_weight,
        value_weight, output_gate_weight, decay_logit_bias.reshape(1, qk),
        extra_log_decay, head_norm_gain.reshape(1, v), attention_out_weight,
        gain_blocks(pre_attention_gain), gain_blocks(post_attention_gain),
        gain_blocks(pre_feedforward_gain), gain_blocks(post_feedforward_gain),
        up_weight, down_weight,
    )
    return out.reshape(length, width)


def local(*arrays):
    n_fs, n_tp, n_grp = (lax.axis_size(name) for name in ("fs", "tp", "grp"))
    length, width = arrays[0].shape
    units = arrays[-2].shape[1]
    fits = n_fs == 4 and n_grp == 2 and n_tp == 4 and width // n_fs % 128 == 0
    fits = fits and length % (n_tp * 16) == 0 and arrays[2].shape[1] % 128 == 0
    fits = fits and units % 512 == 0 and width // n_fs == units // n_fs
    return local_fused(*arrays) if fits else local_plain(*arrays)


def solution(mesh):
    return jax.shard_map(
        local,
        mesh=mesh,
        in_specs=(
            P(("grp", "fs"), None), P(), P("fs", "tp"), P("fs", "tp"), P("fs", "tp"),
            P("fs", "tp"), P("fs", "tp"), P("tp"), P(("grp", "fs"), "tp"), P("tp"),
            P("tp", "fs"), P(), P(), P(), P("fs", "tp"), P("tp", "fs"),
        ),
        out_specs=P(("grp", "fs"), None),
        check_vma=False,
    )
```

```python
import math

import jax
import jax.numpy as jnp
from jax import lax
from jax.experimental import pallas as pl
from jax.experimental.pallas import tpu as pltpu
from jax.sharding import PartitionSpec as P

DK = 64
DV = 128
EPS = 1e-06
GATE_NORM_SCALE = 16.0
VMEM_LIMIT = 60 * 2**20


def root_norm(rows, gain):
    return rows * lax.rsqrt(jnp.mean(rows * rows, axis=-1, keepdims=True) + EPS) * gain


def split2(x):
    hi = x.astype(jnp.bfloat16)
    lo = (x - hi.astype(jnp.float32)).astype(jnp.bfloat16)
    return hi, lo


def dot_t(a, b):
    return lax.dot_general(a, b, (((1,), (1,)), ((), ())), preferred_element_type=jnp.float32)


def split3(x):
    hi = x.astype(jnp.bfloat16)
    rest = x - hi.astype(jnp.float32)
    mid = rest.astype(jnp.bfloat16)
    return hi, mid, (rest - mid.astype(jnp.float32)).astype(jnp.bfloat16)


def pick(mask, parts):
    chosen = mask.astype(jnp.float32).astype(jnp.bfloat16)
    total = 0.0
    for part in parts:
        total = total + jnp.dot(chosen, part, preferred_element_type=jnp.float32)
    return total


def attend(q, k, v, log_decay):
    n, width = q.shape
    heads = width // DK
    row = lax.broadcasted_iota(jnp.int32, (n, n), 0)
    col = lax.broadcasted_iota(jnp.int32, (n, n), 1)
    lane = lax.broadcasted_iota(jnp.int32, (n, width), 1)
    cum = pick(row >= col, split3(log_decay))
    cum_parts = split3(cum)

    def per_head(x):
        return jnp.concatenate(
            [jnp.where((lane >= h * DK) & (lane < (h + 1) * DK), x, 0.0) for h in range(heads)], 0
        )

    def scores_of(left, right):
        lh, ll = split2(per_head(left))
        rh, rl = split2(right)
        return dot_t(lh, rh) + dot_t(lh, rl) + dot_t(ll, rh)

    tiled_row = jnp.concatenate([row] * heads, 0)
    tiled_col = jnp.concatenate([col] * heads, 0)
    scores = jnp.where(
        tiled_row == tiled_col,
        dot_t(per_head(q).astype(jnp.bfloat16), k.astype(jnp.bfloat16)),
        0.0,
    )
    half = n // 2
    while half >= 1:
        bound = pick(col == (row & ~(2 * half - 1)) + (half - 1), cum_parts)
        fade = jnp.exp(-jnp.abs(cum - bound))
        part = scores_of(q * fade, k * fade)
        apart = tiled_row ^ tiled_col
        keep = (apart >= half) & (apart < 2 * half) & (tiled_row > tiled_col)
        scores = jnp.where(keep, part, scores)
        half //= 2
    outs = []
    for h in range(heads):
        sh, sl = split2(scores[h * n : (h + 1) * n])
        vh = v[:, h * DV : (h + 1) * DV]
        outs.append(
            jnp.dot(sh, vh, preferred_element_type=jnp.float32)
            + jnp.dot(sl, vh, preferred_element_type=jnp.float32)
        )
    return outs


def head_block(acc, bias, extra, gain, qk, v):
    bf = jnp.bfloat16
    q = acc[:, :qk].astype(bf).astype(jnp.float32) * DK ** (-0.5)
    k = acc[:, qk : 2 * qk].astype(bf).astype(jnp.float32)
    x = acc[:, 2 * qk : 3 * qk] + bias
    log_sig = jnp.minimum(x, 0.0) - jnp.log1p(jnp.exp(-jnp.abs(x)))
    rate = log_sig / GATE_NORM_SCALE + extra
    vals = acc[:, 3 * qk : 3 * qk + v].astype(bf)
    gate = acc[:, 3 * qk + v :].astype(bf).astype(jnp.float32)
    outs = attend(q, k, vals, rate)
    scaled = jnp.concatenate(
        [o * lax.rsqrt(jnp.mean(o * o, axis=-1, keepdims=True) + EPS) for o in outs], 1
    )
    return (scaled * gain * (gate / (1.0 + jnp.exp(-gate)))).astype(bf)


def local_plain(
    tokens, pre_attention_gain, query_weight, key_weight, value_weight, output_gate_weight,
    decay_weight, decay_logit_bias, extra_log_decay, head_norm_gain, attention_out_weight,
    post_attention_gain, pre_feedforward_gain, post_feedforward_gain, up_weight, down_weight,
):
    bf = jnp.bfloat16
    n_fs = lax.axis_size("fs")
    n_tp = lax.axis_size("tp")
    length, width = tokens.shape
    share = length // n_tp
    cols = width // n_fs
    qk, v = query_weight.shape[1], value_weight.shape[1]
    stream_in = tokens.astype(jnp.float32)
    normed = root_norm(stream_in, pre_attention_gain).astype(bf)
    joined = jnp.concatenate(
        [query_weight, key_weight, decay_weight, value_weight, output_gate_weight], 1
    )
    whole = lax.all_gather(joined, "fs", axis=0, tiled=True)
    acc = jnp.dot(normed, whole, preferred_element_type=jnp.float32)
    headout = head_block(acc, decay_logit_bias, extra_log_decay, head_norm_gain, qk, v)
    whole_out = lax.all_gather(attention_out_weight, "fs", axis=1, tiled=True)
    mix_part = jnp.dot(headout, whole_out, preferred_element_type=jnp.float32).astype(bf)
    mix = lax.all_to_all(
        mix_part.reshape(n_tp, share, width), "tp", split_axis=0, concat_axis=0, tiled=True
    )
    mixed = jnp.sum(mix.astype(jnp.float32), 0)
    mine = lax.dynamic_slice_in_dim(stream_in, lax.axis_index("tp") * share, share, 0)
    stream = mine + root_norm(mixed, post_attention_gain)
    normed_mid = root_norm(stream, pre_feedforward_gain).astype(bf)
    blocks = normed_mid.reshape(share, n_fs, cols).transpose(1, 0, 2)
    blocks = lax.all_to_all(blocks, "fs", split_axis=0, concat_axis=0, tiled=True)
    rows = lax.all_gather(blocks, "tp", axis=1, tiled=True)
    up = jnp.dot(rows.reshape(n_fs * length, cols), up_weight, preferred_element_type=jnp.float32)
    up = up.astype(bf).reshape(n_fs, length, -1)
    up = lax.all_to_all(up, "fs", split_axis=0, concat_axis=0, tiled=True)
    hidden = jnp.square(jax.nn.relu(jnp.sum(up.astype(jnp.float32), 0))).astype(bf)
    hidden = lax.all_gather(hidden, "fs", axis=0, tiled=True)
    down = jnp.dot(hidden, down_weight, preferred_element_type=jnp.float32).astype(bf)
    down = down.reshape(n_fs, n_tp, share, cols).transpose(1, 0, 2, 3)
    down = lax.all_to_all(down, "tp", split_axis=0, concat_axis=0, tiled=True)
    feed = jnp.sum(down.astype(jnp.float32), 0).astype(bf)
    feed = lax.all_to_all(feed, "fs", split_axis=0, concat_axis=0, tiled=True)
    feed = feed.transpose(1, 0, 2).reshape(share, width).astype(jnp.float32)
    out = (stream + root_norm(feed, post_feedforward_gain)).astype(bf)
    return lax.all_gather(out, "tp", axis=0, tiled=True)


def exchange_kernel(
    x_ref, q_ref, k_ref, d_ref, v_ref, g_ref, bias_ref, extra_ref, head_gain_ref, wo_ref,
    gain_a_ref, gain_b_ref, gain_c_ref, gain_d_ref, up_ref, down_ref, out_ref,
    nm, no, qp, kp, dp, vp, gp, p1s, p2s, p1r, p2r, wop, mixs, mixr, st, am, upf, dnf, hid,
    part, from_sib, to_x, from_x, to_pair, from_pair, to_far, from_far, to_late, from_late, ff,
    done, here, send, recv,
    *, n_fs, n_tp, qk, v, loads,
):
    bf, f32 = jnp.bfloat16, jnp.float32
    g, f, t = lax.axis_index("grp"), lax.axis_index("fs"), lax.axis_index("tp")
    pair, far, b, half = f ^ 1, f ^ 2, f & 1, f >> 1
    inner = (b ^ half) == 1
    share = out_ref.shape[1]
    cols = st.shape[2]
    length = n_tp * share
    count = [0]
    groups = {}

    def slots(n):
        first = count[0]
        count[0] += n
        return first

    def put(src, dst, at, group, again=False, **where):
        sem, sizes = groups.setdefault(group, (len(groups), []))
        if not again:
            sizes.append(math.prod(src.shape))
        pltpu.make_async_remote_copy(
            src_ref=src, dst_ref=dst, send_sem=send.at[sem], recv_sem=recv.at[at],
            device_id=where, device_id_type=pl.DeviceIdType.MESH,
        ).start()

    def copy_like(ref, sem, at):
        return pltpu.make_async_remote_copy(
            src_ref=ref, dst_ref=ref, send_sem=send.at[sem], recv_sem=recv.at[at],
            device_id={"fs": far}, device_id_type=pl.DeviceIdType.MESH,
        )

    def take(dst, at):
        copy_like(dst, 0, at).wait_recv()

    def sent(group, like):
        sem, sizes = groups.pop(group)
        groups[(group, "sent")] = (sem, None)
        assert sum(sizes) == math.prod(like.shape), (group, sum(sizes))
        copy_like(like, sem, 0).wait_send()

    def dot(l, r):
        return jnp.dot(l, r, preferred_element_type=f32)

    def squares(blocks):
        total = 0.0
        for block in blocks:
            total = total + jnp.sum(block * block, axis=-1, keepdims=True)
        return lax.rsqrt(total / (n_fs * cols) + EPS)

    def rows_of(ref, at):
        return ref[:, at].reshape(length, cols)

    hid_cols = upf.shape[2]
    for load in loads:
        load.start()
    own_up = pltpu.make_async_copy(
        up_ref.at[:, pl.ds(pl.multiple_of(f * hid_cols, hid_cols), hid_cols)], upf.at[f], here.at[0]
    )
    own_down = pltpu.make_async_copy(
        down_ref.at[pl.ds(pl.multiple_of(f * hid_cols, hid_cols), hid_cols)], dnf.at[f], here.at[1]
    )

    barrier = pltpu.get_barrier_semaphore()
    peers = [{"grp": 1 - g}]
    peers += [{"fs": f ^ s} for s in range(1, n_fs)]
    peers += [{"tp": t ^ k} for k in range(1, n_tp)]
    for peer in peers:
        pl.semaphore_signal(barrier, inc=1, device_id=peer, device_id_type=pl.DeviceIdType.MESH)
    pl.semaphore_wait(barrier, len(peers))
    for load in loads:
        load.wait()
    own_up.start()
    own_down.start()

    class Fetch:
        def __init__(self, ref, into, pieces, group):
            self.ref, self.into, self.pieces, self.group = ref, into, pieces, group
            self.at = slots(pieces + 1)
            self.size = ref.shape[0] // (2 * pieces)

        def piece(self, ref, side, i):
            at = pl.multiple_of(side * (self.pieces * self.size) + i * self.size, self.size)
            return ref.at[pl.ds(at, self.size)]

        def start(self):
            for i in range(self.pieces):
                put(
                    self.piece(self.ref, g, i), self.piece(self.into, g, i), self.at + 1 + i,
                    self.group, fs=pair,
                )

        def pass_on(self):
            for i in range(self.pieces):
                mine = self.piece(self.into, g, i)
                take(mine, self.at + 1 + i)
                put(mine, mine, self.at, self.group, grp=1 - g)

        def settle(self):
            rows = self.pieces * self.size
            take(self.into.at[pl.ds(pl.multiple_of((1 - g) * rows, rows), rows)], self.at)

    class Spread:
        def __init__(self, source, spot, group, fine):
            self.source, self.spot, self.group, self.fine = source, spot, group, fine
            self.pieces = 2
            self.at = slots(n_fs * (self.pieces + 1))
            self.tail = slots(1)
            self.size = hid_cols // (2 * self.pieces)

        def sem(self, s, i):
            return self.at + s * (self.pieces + 1) + i

        def parts(self, s, i):
            halves = [(pl.ds(0, hid_cols // 2), self.sem(s, i))]
            halves.append((pl.ds(hid_cols // 2, hid_cols // 2), self.tail))
            return halves if self.fine and (s, i) == (3, 1) else [(pl.ds(0, hid_cols), self.sem(s, i))]

        def chunk(self, side, i):
            return pl.ds(pl.multiple_of((side * self.pieces + i) * self.size, self.size), self.size)

        def start(self, s, i, again=False):
            at = self.chunk(g, i)
            for span, sem in self.parts(s, i):
                put(
                    self.source(f ^ s, at, span), self.spot(f, at, span), sem, self.group, again,
                    fs=f ^ s,
                )

        def inner_start(self, s, i, again=False):
            pl.when(inner)(lambda: self.start(s, i, again))

        def outer_start(self, s, i, again=True):
            pl.when(jnp.logical_not(inner))(lambda: self.start(s, i, again))

        def pass_on(self, s, i):
            for span, sem in self.parts(s, i):
                mine = self.spot(f ^ s, self.chunk(g, i), span)
                take(mine, sem)
                put(mine, mine, self.sem(s, self.pieces), self.group, grp=1 - g)

        def settle(self, s):
            wide = self.pieces * self.size
            at = pl.ds(pl.multiple_of((1 - g) * wide, wide), wide)
            take(self.spot(f ^ s, at, pl.ds(0, hid_cols)), self.sem(s, self.pieces))

    def units_of(to):
        return pl.ds(pl.multiple_of(to * hid_cols, hid_cols), hid_cols)

    def up_source(to, at, span):
        return up_ref.at[at, units_of(to)]

    def down_source(to, at, span):
        first = pl.multiple_of(to * hid_cols + span.start, hid_cols // 2)
        return down_ref.at[pl.ds(first, span.size), at]

    up = Spread(up_source, lambda c, at, span: upf.at[c, at], "up", False)
    down = Spread(down_source, lambda c, at, span: dnf.at[c, span, at], "down", True)
    weights = [q_ref, k_ref, d_ref, v_ref, g_ref]
    fetches = [
        Fetch(r, p, n, group)
        for r, p, n, group in zip(
            weights, (qp, kp, dp, vp, gp), (1, 1, 1, 2, 2), ("qk", "qk", "qk", "v", "v")
        )
    ]

    def normalize(rows, into, at):
        blocks = [rows[:, c * cols : (c + 1) * cols].astype(f32) for c in range(n_fs)]
        scale = squares(blocks)
        for c in range(n_fs):
            into[at, c] = (blocks[c] * scale * gain_a_ref[c]).astype(bf)

    wo_at = slots(n_fs)
    rows_wo = wo_ref.shape[0] // 2

    def wo_part(ref, side):
        return ref.at[pl.ds(pl.multiple_of(side * rows_wo, rows_wo), rows_wo)]

    def wo_start(s):
        put(wo_part(wo_ref, g), wo_part(wop.at[f], g), wo_at + s, "wo", fs=f ^ s)

    def wo_pass(s):
        mine = wo_part(wop.at[f ^ s], g)
        take(mine, wo_at + s)
        if s == 2:
            put(mine, mine, wo_at + 3, "wo", fs=pair)
        put(mine, mine, wo_at, "wo", grp=1 - g)

    normalize(x_ref[t], nm, t)
    no_at = slots(2)
    put(nm.at[t, pl.ds(2 * (1 - half), 2)], no.at[t], no_at, "no", fs=far)
    for fetch in fetches:
        fetch.start()
    up.inner_start(3, 0)
    up.inner_start(3, 1)
    wo_start(2)
    wo_start(1)
    for k in range(1, n_tp):
        normalize(x_ref[t ^ k], nm, t ^ k)

    fetches[0].pass_on()
    take(no.at[t], no_at)
    for k in (2, 3, 1):
        put(no.at[t], no.at[t], no_at + 1, "no", tp=t ^ k)
    fetches[1].pass_on()
    fetches[2].pass_on()
    take(no.at[pl.ds(0, n_tp - 1)], no_at + 1)
    no_own, no_pair = rows_of(no, b), rows_of(no, 1 - b)
    outgoing = [p1s.at[0], p1s.at[1], p1s.at[2], p2s.at[0], p2s.at[1]]
    incoming = [p1r.at[0], p1r.at[1], p1r.at[2], p2r.at[0], p2r.at[1]]
    part_at = slots(2)

    def far_part(i):
        fetches[i].settle()
        outgoing[i][...] = (
            dot(no_own, weights[i][...]) + dot(no_pair, fetches[i].into[...])
        ).astype(bf)
        late = i // 3
        put(outgoing[i], incoming[i], part_at + late, ("p1", "p2")[late], fs=far)

    far_part(0)
    far_part(1)
    fetches[3].pass_on()
    far_part(2)
    fetches[4].pass_on()
    nm_own, nm_pair = rows_of(nm, f), rows_of(nm, pair)

    def own_part(i):
        return dot(nm_own, weights[i][...]) + dot(nm_pair, fetches[i].into[...])

    acc = [own_part(0), own_part(1), own_part(2)]
    far_part(3)
    wo_pass(2)
    far_part(4)
    wo_pass(1)
    for s, i in ((1, 0), (1, 1), (2, 0)):
        up.start(s, i)
    up.outer_start(3, 0)
    up.start(2, 1)
    up.outer_start(3, 1)
    acc += [own_part(3), own_part(4)]
    take(p1r, part_at)
    wo_pass(3)
    take(p2r, part_at + 1)
    acc = [mine + other[...].astype(f32) for mine, other in zip(acc, incoming)]
    headout = head_block(
        jnp.concatenate(acc, 1), bias_ref[...], extra_ref[...], head_gain_ref[...], qk, v
    )

    def mix_block(s):
        weight = wo_ref[...] if s == 0 else wop[f ^ s]
        block = dot(headout, weight).astype(bf)
        for k in range(n_tp):
            mixs[k ^ t, f ^ s] = block[k * share : (k + 1) * share]

    mix_block(0)
    take(wop.at[pl.ds(0, n_fs - 1), pl.ds(0, rows_wo)], wo_at)
    for s in (1, 2, 3):
        mix_block(s)
    mix_at = slots(n_tp)
    put(mixs.at[3], mixr.at[3], mix_at + 3, "mix", tp=t ^ 1)
    put(mixs.at[1], mixr.at[1], mix_at + 1, "mix", tp=t ^ 1)
    up.pass_on(1, 0)
    take(mixr.at[3], mix_at + 3)
    mixr[0] = (mixs[2].astype(f32) + mixr[3].astype(f32)).astype(bf)
    put(mixr.at[0], mixr.at[2], mix_at + 2, "mix", tp=t ^ 2)
    mine = [x_ref[t, :, c * cols : (c + 1) * cols].astype(f32) for c in range(n_fs)]
    up.pass_on(1, 1)
    take(mixr.at[1], mix_at + 1)
    take(mixr.at[2], mix_at + 2)
    mix = mixs[0].astype(f32) + mixr[1].astype(f32) + mixr[2].astype(f32)
    mix = [mix[c] for c in range(n_fs)]
    scale = squares(mix)
    stream = [mine[c] + mix[c] * scale * gain_b_ref[c] for c in range(n_fs)]
    scale = squares(stream)
    for c in range(n_fs):
        st[c] = stream[c]
        am[0, 0, c] = (stream[c] * scale * gain_c_ref[c]).astype(bf)

    mid_z, mid_x, mid_sib = slots(n_fs), slots(n_fs), slots(n_fs)

    def mid_over(k):
        put(am.at[k, 0], am.at[k, 2], mid_x + k, "mid", tp=t ^ 2)
        put(am.at[k, 0], am.at[k, 1], mid_sib + k, "mid", tp=t ^ 1)

    def mid_across(k):
        take(am.at[k, 2], mid_x + k)
        put(am.at[k, 2], am.at[k, 3], mid_sib + k, "mid", tp=t ^ 1)

    put(am.at[0, 0], am.at[2, 0], mid_z + 2, "mid_z", fs=far)
    put(am.at[0, 0], am.at[1, 0], mid_z + 1, "mid_z", fs=pair)
    mid_over(0)
    down.inner_start(3, 0)
    down.inner_start(3, 1)
    up.pass_on(2, 0)
    up.pass_on(3, 0)
    up.pass_on(2, 1)
    take(am.at[2, 0], mid_z + 2)
    put(am.at[2, 0], am.at[3, 0], mid_z + 3, "mid_z", fs=pair)
    mid_over(2)
    down.start(1, 0)
    down.start(1, 1)
    for s, i in ((2, 0), (2, 1), (3, 0), (3, 1)):
        down.outer_start(s, i, s == 3)
    take(am.at[1, 0], mid_z + 1)
    mid_over(1)
    up.pass_on(3, 1)
    mid_across(0)
    sent("qk", am.at[0, pl.ds(0, 3)])
    sent("v", am.at[0])
    sent("no", am.at[0, pl.ds(0, 2)])
    sent("wo", wop.at[pl.ds(0, 3)])
    sent("p1", p1s)
    sent("p2", p2s)
    sent("mix", mixs.at[pl.ds(0, 3)])
    take(am.at[3, 0], mid_z + 3)
    mid_over(3)
    down.inner_start(2, 0, True)
    down.inner_start(2, 1, True)
    mid_across(2)
    mid_across(1)
    for s in (1, 2, 3):
        up.settle(s)
    own_up.wait()

    def raise_rows(k):
        take(am.at[k, pl.ds(0, 2)], mid_sib + k)
        total = 0.0
        for c in range(n_fs):
            total = total + dot(am[k, :, c].reshape(length, cols), upf[c])
        total = jnp.maximum(total, 0.0)
        hid[k] = (total * total).astype(bf)

    raise_rows(0)
    raise_rows(2)
    down.pass_on(1, 0)
    raise_rows(1)
    mid_across(3)
    down.pass_on(1, 1)
    raise_rows(3)
    own_down.wait()

    sib_at, x3_at, x_at = slots(2 * n_fs), slots(2 * n_fs), slots(2 * n_fs)
    pair_at, far_at, late_at = slots(2), slots(2) - 2, slots(4)
    hidden = hid[...].reshape(n_fs * length, hid_cols)
    wide = cols // 2

    def columns(side):
        at = g if side == 0 else 1 - g
        return pl.ds(pl.multiple_of(at * wide, wide), wide)

    def project(j, side):
        both = (0, 1) if side is None else (side,)
        for one in both:
            block = dot(hidden, dnf[f ^ j, :, columns(one)]).astype(bf)
            block = block.reshape(n_fs, n_tp, share, wide)
            for m in range(n_tp):
                part[j, m, one] = block[:, m]
        at = pl.ds(0, 2) if side is None else pl.ds(side, 1)
        sem = 2 * j + (side or 0)
        put(part.at[j, 3, at], from_sib.at[j, 1, at], x3_at + sem, "sib", tp=t ^ 1)
        put(part.at[j, 1, at], from_sib.at[j, 0, at], sib_at + sem, "sib", tp=t ^ 1)

    def over_x(j, side):
        at = pl.ds(0, 2) if side is None else pl.ds(side, 1)
        sem = 2 * j + (side or 0)
        take(from_sib.at[j, 1, at], x3_at + sem)
        to_x[j, at] = (part[j, 2, at].astype(f32) + from_sib[j, 1, at].astype(f32)).astype(bf)
        put(to_x.at[j, at], from_x.at[j, at], x_at + sem, "x", tp=t ^ 2)

    def summed(j, side, k):
        total = part[j, 0, side, k].astype(f32) + from_sib[j, 0, side, k].astype(f32)
        return total + from_x[j, side, k].astype(f32)

    def over_pair(j):
        take(from_sib.at[j, 0], sib_at + 2 * j)
        take(from_x.at[j], x_at + 2 * j)
        for k in (1, 3):
            for side in range(2):
                to_pair[j, k >> 1, side] = summed(j, side, k).astype(bf)
        put(to_pair.at[j], from_pair.at[j ^ 1], pair_at + (j ^ 1), "pair", fs=pair)
        for k in (0, 2):
            for side in range(2):
                ff[j, k >> 1, side] = summed(j, side, k)

    def over_far(j):
        take(from_pair.at[j], pair_at + j)
        to_far[j] = (ff[j, 1] + from_pair[j, 1].astype(f32)).astype(bf)
        put(to_far.at[j], from_far.at[j ^ 2], far_at + (j ^ 2), "far", fs=far)

    def direct(j, side):
        at = pl.ds(side, 1)
        take(from_sib.at[j, 0, at], sib_at + 2 * j + side)
        take(from_x.at[j, at], x_at + 2 * j + side)
        for k in (3, 2, 1):
            to_late[j - 2, side, k] = summed(j, side, k).astype(bf)
            put(
                to_late.at[j - 2, side, k], from_late.at[j - 2, side, k],
                late_at + 2 * (j - 2) + side, "late", fs=f ^ k,
            )
        ff[j, 0, side] = summed(j, side, 0)

    project(0, None)
    down.pass_on(2, 0)
    down.settle(1)
    project(1, None)
    over_x(0, None)
    down.pass_on(2, 1)
    over_x(1, None)
    project(2, 0)
    over_pair(0)
    down.pass_on(3, 0)
    over_x(2, 0)
    over_pair(1)
    down.settle(2)
    project(2, 1)
    down.pass_on(3, 1)
    project(3, 0)
    over_x(2, 1)
    over_x(3, 0)
    sent("up", upf.at[pl.ds(0, 3)])
    sent("mid", am.at[pl.ds(0, 3)])
    sent("mid_z", am.at[0, pl.ds(0, 3)])
    direct(2, 0)
    down.settle(3)
    project(3, 1)
    direct(2, 1)
    over_x(3, 1)
    over_far(0)
    over_far(1)
    direct(3, 0)
    sent("pair", to_pair.at[pl.ds(0, 2)])
    feed = [[ff[j, 0, side] for side in range(2)] for j in range(n_fs - 1)]
    feed.append([ff[3, 0, 0], None])
    for j in (0, 1):
        for side in range(2):
            feed[j][side] = feed[j][side] + from_pair[j, 0, side].astype(f32)
    for j in (2, 3):
        take(from_far.at[j], far_at + j)

    def add_late(j, side):
        take(from_late.at[j - 2, side, pl.ds(0, 3)], late_at + 2 * (j - 2) + side)
        for k in (1, 2, 3):
            feed[j ^ k][side] = feed[j ^ k][side] + from_late[j - 2, side, k].astype(f32)

    sent("down", dnf.at[pl.ds(0, 3)])
    sent("far", to_far.at[pl.ds(0, 2)])
    direct(3, 1)
    feed[3][1] = ff[3, 0, 1]
    for j in (2, 3):
        for side in range(2):
            feed[j][side] = feed[j][side] + from_far[j, side].astype(f32)
    for j, side in ((2, 0), (2, 1), (3, 0)):
        add_late(j, side)
    sent("sib", part.at[pl.ds(0, 2)])
    sent("x", to_x)
    add_late(3, 1)
    scale = squares([block for blocks in feed for block in blocks])
    for j in range(n_fs):
        for side in range(2):
            at = pl.ds(pl.multiple_of((f ^ j) * cols + (g ^ side) * wide, wide), wide)
            gained = feed[j][side] * scale * gain_d_ref[f ^ j, :, columns(side)]
            done[0, :, at] = (st[f ^ j, :, columns(side)] + gained).astype(bf)
    out_at = slots(4)
    kept = [
        pltpu.make_async_copy(done.at[0], out_ref.at[t], here.at[0]),
        pltpu.make_async_copy(done.at[1], out_ref.at[t ^ 2], here.at[1]),
    ]
    put(done.at[0], done.at[1], out_at, "out", tp=t ^ 2)
    put(done.at[0], out_ref.at[t], out_at + 1, "out", tp=t ^ 1)
    kept[0].start()
    sent("late", no.at[pl.ds(0, 3)])
    take(done.at[1], out_at)
    put(done.at[1], out_ref.at[t ^ 2], out_at + 2, "out", tp=t ^ 1)
    kept[1].start()
    kept[0].wait()
    take(out_ref.at[t ^ 1], out_at + 1)
    kept[1].wait()
    take(out_ref.at[t ^ 3], out_at + 2)
    sent("out", mixs.at[pl.ds(0, 3)])
    assert count[0] <= recv.shape[0] and len(groups) <= send.shape[0], (count, len(groups))


def local_fused(
    tokens, pre_attention_gain, query_weight, key_weight, value_weight, output_gate_weight,
    decay_weight, decay_logit_bias, extra_log_decay, head_norm_gain, attention_out_weight,
    post_attention_gain, pre_feedforward_gain, post_feedforward_gain, up_weight, down_weight,
):
    bf, f32 = jnp.bfloat16, jnp.float32
    n_fs, n_tp = lax.axis_size("fs"), lax.axis_size("tp")
    length, width = tokens.shape
    share, cols = length // n_tp, width // n_fs
    qk, v = query_weight.shape[1], value_weight.shape[1]
    mine = up_weight.shape[1] // n_fs
    vm = pltpu.VMEM
    block = (n_fs, share, cols)
    sides, rows = (2,), (n_fs, share, cols // 2)
    scratch = [
        vm((n_tp,) + block, bf), vm((n_tp, 2, share, cols), bf),
        vm(query_weight.shape, bf), vm(key_weight.shape, bf), vm(decay_weight.shape, bf),
        vm(value_weight.shape, bf), vm(output_gate_weight.shape, bf),
        vm((3, length, qk), bf), vm((2, length, v), bf),
        vm((3, length, qk), bf), vm((2, length, v), bf),
        vm((n_fs,) + attention_out_weight.shape, bf),
        vm((n_tp,) + block, bf), vm((n_tp,) + block, bf), vm(block, f32),
        vm((n_fs, n_tp) + block, bf),
        vm((n_fs, cols, mine), bf), vm((n_fs, mine, cols), bf),
        vm((n_fs, length, mine), bf),
        vm((n_fs, n_tp) + sides + rows, bf), vm((n_fs, 2) + sides + rows, bf),
        vm((n_fs,) + sides + rows, bf), vm((n_fs,) + sides + rows, bf),
        vm((n_fs, 2, 2) + rows[1:], bf), vm((n_fs, 2, 2) + rows[1:], bf),
        vm((n_fs, 2) + rows[1:], bf), vm((n_fs, 2) + rows[1:], bf),
        vm((2,) + sides + rows, bf), vm((2,) + sides + rows, bf),
        vm((n_fs, 2, 2) + rows[1:], f32),
        vm((2, share, width), bf), pltpu.SemaphoreType.DMA((2,)),
        pltpu.SemaphoreType.DMA((20,)), pltpu.SemaphoreType.DMA((100,)),
    ]

    inputs = [
        tokens.reshape(n_tp, share, width), query_weight, key_weight, decay_weight,
        value_weight, output_gate_weight, decay_logit_bias.reshape(1, qk),
        extra_log_decay, head_norm_gain.reshape(1, v), attention_out_weight,
    ] + [
        gain.reshape(n_fs, 1, cols)
        for gain in (
            pre_attention_gain, post_attention_gain, pre_feedforward_gain, post_feedforward_gain
        )
    ]
    staged = len(inputs)

    def kernel(*refs):
        far_refs, rest, near_refs = refs[:staged], refs[staged : -staged - 1], refs[-staged - 1 : -1]
        loads = [
            pltpu.make_async_copy(source, into, refs[-1].at[i])
            for i, (source, into) in enumerate(zip(far_refs, near_refs))
        ]
        exchange_kernel(
            *near_refs, *rest, n_fs=n_fs, n_tp=n_tp, qk=qk, v=v, loads=loads
        )

    scratch += [vm(array.shape, array.dtype) for array in inputs]
    scratch.append(pltpu.SemaphoreType.DMA((staged,)))
    out = pl.pallas_call(
        kernel,
        out_shape=jax.ShapeDtypeStruct((n_tp, share, width), bf),
        in_specs=[pl.BlockSpec(memory_space=pltpu.HBM)] * (staged + 2),
        out_specs=pl.BlockSpec(memory_space=pltpu.HBM),
        scratch_shapes=scratch,
        compiler_params=pltpu.CompilerParams(
            collective_id=0, has_side_effects=True, vmem_limit_bytes=VMEM_LIMIT
        ),
    )(*inputs, up_weight, down_weight)
    return out.reshape(length, width)


def local(*arrays):
    n_fs, n_tp, n_grp = (lax.axis_size(name) for name in ("fs", "tp", "grp"))
    length, width = arrays[0].shape
    units = arrays[-2].shape[1]
    fits = n_fs == 4 and n_grp == 2 and n_tp == 4 and width // n_fs % 128 == 0
    fits = fits and length % (n_tp * 16) == 0 and arrays[2].shape[1] % 128 == 0
    fits = fits and units % 512 == 0 and width // n_fs == units // n_fs
    return local_fused(*arrays) if fits else local_plain(*arrays)


def solution(mesh):
    return jax.shard_map(
        local,
        mesh=mesh,
        in_specs=(
            P(("grp", "fs"), None), P(), P("fs", "tp"), P("fs", "tp"), P("fs", "tp"),
            P("fs", "tp"), P("fs", "tp"), P("tp"), P(("grp", "fs"), "tp"), P("tp"),
            P("tp", "fs"), P(), P(), P(), P("fs", "tp"), P("tp", "fs"),
        ),
        out_specs=P(("grp", "fs"), None),
        check_vma=False,
    )
```
